32 devices in a mesh: fs: 4 (over z), tp: 8 (over y, x, core).
Axes of the slice: x: 2, y: 2, z: 4, core: 2. Of those that a mesh axis runs over, the one named last changes fastest.
Arguments:
- tokens: bfloat16 [768, 2304], P('fs'), may hold values from -6 to 6
- gate_train: float32 [8, 2304, 2304], P(None, 'fs', 'tp'), may hold values from -0.125 to 0.125
- up_train: float32 [8, 2304, 2304], P(None, 'fs', 'tp'), may hold values from -0.125 to 0.125
- down_train: float32 [8, 2304, 2304], P(None, 'fs', 'tp'), may hold values from -0.125 to 0.125
- gain: float32 [2304], P('fs'), may hold values from 0.1 to 1.9
- routes: int32 [768, 2], P('fs'), may hold values from 0 to 7, all different within a row; in each aligned block of 192 rows (0 to 191, 192 to 383, ...) at most 72 rows name the same one
- route_weights: float32 [768, 2], P('fs'), may hold values from 0.1 to 1
Outputs:
- gate_new: bfloat16 [8, 2304, 2304], P('tp')
- up_new: bfloat16 [8, 2304, 2304], P('tp')
- down_new: bfloat16 [8, 2304, 2304], P('tp')
- mixed: bfloat16 [768, 2304], P('fs', 'tp')
The draws below stay inside these ranges and needn't reach their ends.
Inputs may be any that keep to these rules, and one draw needn't show every extreme that they name: `routes`: each row names two different experts; in each aligned block of 192 rows at most 72 rows name one expert, a bound that some block reaches.
All inputs are finite; a program needn't handle non-finite values.
Results may differ from the reference program's by a relative error of at most 0.0095.
Values may be sent and summed in bfloat16 or wider, within the bound.
A program may use at most 128 MiB of HBM per device.

```python
import math
import jax
import jax.numpy as jnp
import numpy as np
from jax import lax

D = 2304
FF = 2304
EXPERTS = 8
ROWS = 192
CAP = 72
TOKENS = 768
N_FS = 4
N_TP = 8


def levels(own_key, shape, pieces, smallest, largest):
    level, own = 1.0, jax.random.fold_in(own_key, 6)
    for position, shards_of in pieces:
        heights = jnp.exp(jax.random.uniform(jax.random.fold_in(own, position), (shards_of,), jnp.float32, smallest / len(pieces), largest / len(pieces)))
        level = level * jnp.repeat(heights, shape[position] // shards_of).reshape([-1 if axis == position else 1 for axis in range(len(shape))])
    return level


def routed_block(own_key, own, number, rows, number_of, top, most, lean):
    sequence = jax.random.permutation(own_key, number_of)
    packed, usual = load_shares(number_of, rows * top, most, lean, True), load_shares(number_of, rows * top, most, lean, False)
    places = jnp.arange(number_of)

    def named(lengths, rotation):
        used = int((lengths > 0).sum())
        fixed = max(1, used // 4)
        passed = fixed + (places - fixed + rotation * (used - fixed)) % max(1, number_of - fixed)
        return jnp.zeros((number_of,), jnp.int32).at[sequence[jnp.where(places < fixed, places, passed)]].set(jnp.asarray(lengths, jnp.int32))

    lengths = jnp.where(number % 4 == 0, named(packed, number // 4), named(usual, number - number // 4 - 1))
    mixed = jax.random.permutation(jax.random.fold_in(own, 3), number_of)
    giver, receiver = mixed[0:number_of // 2 * 2:2], mixed[1:number_of // 2 * 2:2]
    margin = jnp.minimum(lengths[giver] - 1, most - lengths[receiver]) // 2
    margin = jnp.where((giver == sequence[0]) | (receiver == sequence[0]) | (lengths[receiver] == 0), 0, jnp.maximum(margin, 0))
    passed = jax.random.randint(jax.random.fold_in(own, 4), (number_of // 2,), 0, 1 << 20) % (margin + 1)
    lengths = lengths.at[giver].add(-passed).at[receiver].add(passed)
    members = jnp.searchsorted(jnp.cumsum(lengths), jnp.arange(rows * top), side="right").astype(jnp.int32)
    table = members.reshape(top, rows).T
    table = table[jax.random.permutation(jax.random.fold_in(own, 1), rows)]
    rotation = jax.random.randint(jax.random.fold_in(own, 2), (rows, 1), 0, top)
    return jnp.take_along_axis(table, (jnp.arange(top)[None, :] + rotation) % top, axis=1)


def load_shares(count, total, bound, skew, full):
    loads = [(1 << 20) // math.isqrt(rank ** skew) + 1 for rank in range(1, count + 1)]
    largest = bound if full else min(bound, max(-(-total // count), total * loads[0] // sum(loads)))
    least = 1 if total - largest >= count - 1 else 0
    given, rest = [largest] + [least] * (count - 1), total - largest - least * (count - 1)
    while rest > 0:
        free = [i for i in range(1, count) if given[i] < largest] or [i for i in range(1, count) if given[i] < bound]
        pool, remaining = sum([loads[i] for i in free]), rest
        for i in free:
            extra = min(bound - given[i], max(1, remaining * loads[i] // pool), rest)
            given[i] = given[i] + extra
            rest = rest - extra
    return np.array(given)


def scatter_about(stream_key, shape, scale, bound, split=(), kind=jnp.bfloat16):
    array = scale * jax.random.normal(stream_key, shape, jnp.float32)
    if split:
        array = array * levels(stream_key, shape, split, -0.22, 0.18)
    return jnp.clip(array, -bound, bound).astype(kind)


def setup_inputs(seed: int = 0) -> dict:
    keys = jax.random.split(jax.random.key(seed), 8)
    tokens = scatter_about(keys[0], (TOKENS, D), 1.0, 6.0, ((0, 4),))
    gate_train = scatter_about(keys[1], (EXPERTS, D, FF), D ** -0.5, 0.125, ((1, 4), (2, 8)), jnp.float32)
    up_train = scatter_about(keys[2], (EXPERTS, D, FF), D ** -0.5, 0.125, ((1, 4), (2, 8)), jnp.float32)
    down_train = scatter_about(keys[3], (EXPERTS, D, FF), FF ** -0.5, 0.125, ((1, 4), (2, 8)), jnp.float32)
    gain = jnp.clip(1.0 + 0.18 * jax.random.normal(keys[4], (D,), jnp.float32), 0.1, 1.9)
    routes_keys = jax.random.split(jax.random.fold_in(keys[5], 1), TOKENS // ROWS)
    routes_turns = jax.random.permutation(jax.random.fold_in(keys[5], 3), TOKENS // ROWS)
    routes = jax.vmap(lambda own, number: routed_block(jax.random.fold_in(keys[5], 2), own, number, ROWS, EXPERTS, 2, CAP, 1))(routes_keys, routes_turns).reshape((TOKENS, 2))
    route_weights = jnp.clip(0.1 + 0.9 * jax.random.uniform(keys[6], (TOKENS, 2), jnp.float32) ** levels(keys[6], (TOKENS, 2), ((0, 4),), -0.2, 0.2), 0.1, 1.0)
    return dict(tokens=tokens, gate_train=gate_train, up_train=up_train, down_train=down_train, gain=gain, routes=routes, route_weights=route_weights)


norm_eps = 1e-06

def arrange(matrix):
    experts, row_count, col_count = matrix.shape
    slices = N_TP // experts
    piece_width = col_count // (N_TP * slices)
    shaped = matrix.reshape(experts, row_count, N_TP, slices, piece_width)
    return shaped.transpose(0, 3, 2, 4, 1).reshape(experts * slices, col_count // slices, row_count)

def reference(tokens, gate_train, up_train, down_train, gain, routes, route_weights):
    gain_column = gain.astype(jnp.float32)[None, :, None]
    gate_new = arrange((gate_train * gain_column).astype(jnp.bfloat16))
    up_new = arrange((up_train * gain_column).astype(jnp.bfloat16))
    down_new = arrange(down_train.astype(jnp.bfloat16))
    tokens_wide = tokens.astype(jnp.float32)
    normed = (tokens_wide * lax.rsqrt(lax.optimization_barrier(jnp.mean(tokens_wide * tokens_wide, axis=1, keepdims=True)) + norm_eps)).astype(jnp.bfloat16)
    slices = N_TP // EXPERTS

    def one_block(inputs):
        block_rows, block_routes, block_weights = inputs

        def per_expert(expert, output):
            matches = block_routes == expert
            member = jnp.any(matches, axis=1)
            slot_index = (jnp.cumsum(member.astype(jnp.int32)) - 1).astype(jnp.int32)
            marked = jnp.where(member, slot_index, -1)
            picker = (marked[None, :] == jnp.arange(CAP, dtype=jnp.int32)[:, None]).astype(jnp.bfloat16)
            chosen = jnp.dot(picker, block_rows, preferred_element_type=jnp.float32).astype(jnp.bfloat16)
            gate_part = lax.dynamic_slice_in_dim(gate_new, expert * slices, slices, 0).astype(jnp.float32)
            up_part = lax.dynamic_slice_in_dim(up_new, expert * slices, slices, 0).astype(jnp.float32)
            down_part = lax.dynamic_slice_in_dim(down_new, expert * slices, slices, 0).astype(jnp.float32)
            chosen_wide = chosen.astype(jnp.float32)
            gate_pre = jnp.einsum('cd,sfd->scf', chosen_wide, gate_part)
            up_pre = jnp.einsum('cd,sfd->scf', chosen_wide, up_part)
            hidden = (jax.nn.silu(gate_pre) * up_pre).astype(jnp.bfloat16)
            partial_value = jnp.einsum('scf,sfd->scd', hidden.astype(jnp.float32), down_part).astype(jnp.bfloat16)
            slice_total = lax.optimization_barrier(jnp.sum(partial_value.astype(jnp.float32), axis=0))
            row_weight = lax.optimization_barrier(jnp.sum(jnp.where(matches, block_weights, 0.0), axis=1))
            gathered = jnp.take(slice_total, jnp.clip(slot_index, 0, CAP - 1), axis=0)
            return output + jnp.where(member[:, None], row_weight[:, None] * gathered, 0.0)
        return lax.fori_loop(0, EXPERTS, per_expert, jnp.zeros((ROWS, D), jnp.float32)).astype(jnp.bfloat16)
    mixed = lax.map(one_block, (normed.reshape(N_FS, ROWS, D), routes.reshape(N_FS, ROWS, 2), route_weights.reshape(N_FS, ROWS, 2)))
    return (gate_new, up_new, down_new, mixed.reshape(TOKENS, D))
```

```python
import jax
import jax.numpy as jnp
from jax import lax
from jax.experimental import pallas as pl
from jax.experimental.pallas import tpu as pltpu
from jax.sharding import PartitionSpec as P

CAP = 72


norm_eps = 1e-06


def arrange(matrix, tp_count):
    experts, row_count, col_count = matrix.shape
    slices = tp_count // experts
    piece_width = col_count // slices
    shaped = matrix.reshape(experts, row_count, slices, piece_width)
    return shaped.transpose(0, 2, 3, 1).reshape(tp_count, piece_width, row_count)


def block_of(*counts):
    for size in (256, 128):
        if all(count % size == 0 for count in counts):
            return size
    return None


def flip(wide, total_rows, first_row, base=None):
    features, rows = wide.shape
    size = block_of(rows, first_row, total_rows) or rows
    first = first_row // size

    def kernel(*refs):
        refs[-1][...] = refs[0][...].T

    in_specs = [pl.BlockSpec((features, size), lambda i: (0, i))]
    operands = [wide]
    aliases = {}
    if base is not None:
        in_specs.append(pl.BlockSpec(memory_space=pl.ANY))
        operands.append(base)
        aliases = {1: 0}
    return pl.pallas_call(
        kernel,
        grid=(rows // size,),
        in_specs=in_specs,
        out_specs=pl.BlockSpec((size, features), lambda i: (first + i, 0)),
        out_shape=jax.ShapeDtypeStruct((total_rows, features), wide.dtype),
        input_output_aliases=aliases,
        cost_estimate=pl.CostEstimate(
            flops=0, bytes_accessed=4 * features * rows, transcendentals=0
        ),
    )(*operands)


def flip_dot(wide, total_rows, hidden):
    features, rows = wide.shape
    size = block_of(rows, total_rows) or rows
    slots = hidden.shape[0]

    def kernel(wide_ref, hidden_ref, rows_ref, total_ref):
        turned = wide_ref[...].T
        rows_ref[...] = turned

        @pl.when(pl.program_id(0) == 0)
        def _():
            total_ref[...] = jnp.zeros_like(total_ref)

        total_ref[...] += jnp.dot(hidden_ref[...], turned, preferred_element_type=jnp.float32)

    return pl.pallas_call(
        kernel,
        grid=(rows // size,),
        in_specs=[
            pl.BlockSpec((features, size), lambda i: (0, i)),
            pl.BlockSpec((slots, size), lambda i: (0, i)),
        ],
        out_specs=[
            pl.BlockSpec((size, features), lambda i: (i, 0)),
            pl.BlockSpec((slots, features), lambda i: (0, 0)),
        ],
        out_shape=[
            jax.ShapeDtypeStruct((total_rows, features), wide.dtype),
            jax.ShapeDtypeStruct((slots, features), jnp.float32),
        ],
        cost_estimate=pl.CostEstimate(
            flops=2 * slots * features * rows,
            bytes_accessed=4 * features * rows,
            transcendentals=0,
        ),
    )(wide, hidden)


def keep_dot(weights, chosen):
    rows, features = weights.shape
    size = block_of(rows) or rows
    slots = chosen.shape[0]

    def kernel(weights_ref, chosen_ref, rows_ref, product_ref):
        rows_ref[...] = weights_ref[...]
        product_ref[...] = lax.dot_general(
            chosen_ref[...],
            weights_ref[...],
            (((1,), (1,)), ((), ())),
            preferred_element_type=jnp.float32,
        )

    return pl.pallas_call(
        kernel,
        grid=(rows // size,),
        in_specs=[
            pl.BlockSpec((size, features), lambda i: (i, 0)),
            pl.BlockSpec((slots, features), lambda i: (0, 0)),
        ],
        out_specs=[
            pl.BlockSpec((size, features), lambda i: (i, 0)),
            pl.BlockSpec((slots, size), lambda i: (0, i)),
        ],
        out_shape=[
            jax.ShapeDtypeStruct((rows, features), weights.dtype),
            jax.ShapeDtypeStruct((slots, rows), jnp.float32),
        ],
        cost_estimate=pl.CostEstimate(
            flops=2 * slots * features * rows,
            bytes_accessed=4 * features * rows,
            transcendentals=0,
        ),
    )(weights, chosen)


def after(value, *others):
    def kernel(*refs):
        pass

    return pl.pallas_call(
        kernel,
        in_specs=[pl.BlockSpec(memory_space=pl.ANY)] * (1 + len(others)),
        out_specs=pl.BlockSpec(memory_space=pl.ANY),
        out_shape=jax.ShapeDtypeStruct(value.shape, value.dtype),
        input_output_aliases={0: 0},
    )(value, *others)


def shards(tokens, gate_train, up_train, down_train, gain, routes, route_weights):
    tp_count = lax.axis_size("tp")
    experts = gate_train.shape[0]
    slices = tp_count // experts
    gain_column = gain[None, :, None]
    gate_round = (gate_train * gain_column).astype(jnp.bfloat16)
    up_round = (up_train * gain_column).astype(jnp.bfloat16)
    down_round = down_train.astype(jnp.bfloat16)

    def exchange(matrix):
        return lax.all_to_all(matrix, "tp", split_axis=0, concat_axis=1, tiled=True)

    local_features = gate_train.shape[1]
    gate_local = arrange(gate_round, tp_count).transpose(2, 0, 1).reshape(local_features, -1)
    gate_all = lax.all_gather(gate_local, "fs", axis=0, tiled=True)
    features = gate_all.shape[0]

    up_moved = exchange(arrange(up_round, tp_count))[0].T
    down_moved = exchange(arrange(down_round, tp_count))[0].T
    up_wide = lax.all_gather(up_moved, "fs", axis=0, tiled=True)

    units = down_moved.shape[1]
    size = block_of(units) or units
    main = units - size if units > size else units
    down_wide = lax.all_gather(down_moved[:, :main], "fs", axis=0, tiled=True)

    tokens_wide = tokens.astype(jnp.float32)
    normed = (
        tokens_wide
        * lax.rsqrt(jnp.mean(tokens_wide * tokens_wide, axis=1, keepdims=True) + norm_eps)
    ).astype(jnp.bfloat16)
    expert = lax.axis_index("tp") // slices
    matches = routes == expert
    member = jnp.any(matches, axis=1)
    slot_index = jnp.cumsum(member.astype(jnp.int32)) - 1
    marked = jnp.where(member, slot_index, -1)
    picker = (marked[None, :] == jnp.arange(CAP, dtype=jnp.int32)[:, None]).astype(jnp.bfloat16)
    chosen = jnp.dot(picker, normed, preferred_element_type=jnp.float32).astype(jnp.bfloat16)
    contract_last = (((1,), (1,)), ((), ()))

    gate_moved = exchange(gate_all.reshape(features, tp_count, -1).transpose(1, 2, 0))
    gate_new, gate_pre = keep_dot(gate_moved[0], chosen)
    up_new = flip(up_wide, units, 0)
    up_pre = jnp.dot(chosen, up_wide, preferred_element_type=jnp.float32)
    hidden = (jax.nn.silu(gate_pre) * up_pre).astype(jnp.bfloat16)
    down_new, partial_value = flip_dot(down_wide, units, hidden[:, :main])
    if main < units:
        rest_moved = after(down_moved[:, main:], up_new, gate_new, hidden)
        rest_wide = lax.all_gather(rest_moved, "fs", axis=0, tiled=True)
        partial_value = partial_value + lax.dot_general(
            hidden[:, main:], rest_wide, contract_last, preferred_element_type=jnp.float32
        )
        down_new = flip(rest_wide, units, main, down_new)
    partial_value = partial_value.astype(jnp.bfloat16)

    labels = jnp.arange(experts, dtype=jnp.int32)
    member_all = jnp.any(routes[:, :, None] == labels[None, None, :], axis=1)
    slots_all = jnp.cumsum(member_all.astype(jnp.int32), axis=0) - 1
    slot_pair = jnp.take_along_axis(slots_all, routes, axis=1)
    flat_index = slot_pair * experts + routes
    received = lax.all_to_all(
        partial_value.reshape(CAP, tp_count, -1), "tp", split_axis=1, concat_axis=1, tiled=True
    )
    summed = jnp.sum(received.reshape(CAP, experts, slices, -1).astype(jnp.float32), axis=2)
    summed = summed.reshape(CAP * experts, -1)
    picked = jnp.take(summed, flat_index, axis=0)
    mixed = jnp.sum(route_weights[:, :, None] * picked, axis=1)
    return (gate_new[None], up_new[None], down_new[None], mixed.astype(jnp.bfloat16))


def solution(mesh):
    in_specs = (
        P("fs", None),
        P(None, "fs", "tp"),
        P(None, "fs", "tp"),
        P(None, "fs", "tp"),
        P("fs"),
        P("fs", None),
        P("fs", None),
    )
    out_specs = (P("tp", None, None), P("tp", None, None), P("tp", None, None), P("fs", "tp"))
    return jax.shard_map(shards, mesh=mesh, in_specs=in_specs, out_specs=out_specs, check_vma=False)
```

```python
import jax
import jax.numpy as jnp
from jax import lax
from jax.experimental import pallas as pl
from jax.experimental.pallas import tpu as pltpu
from jax.sharding import PartitionSpec as P

CAP = 72


norm_eps = 1e-06


def arrange(matrix, tp_count):
    experts, row_count, col_count = matrix.shape
    slices = tp_count // experts
    piece_width = col_count // slices
    shaped = matrix.reshape(experts, row_count, slices, piece_width)
    return shaped.transpose(0, 2, 3, 1).reshape(tp_count, piece_width, row_count)


def block_of(*counts):
    for size in (256, 128):
        if all(count % size == 0 for count in counts):
            return size
    return None


def flip(wide, total_rows, first_row, base=None):
    features, rows = wide.shape
    size = block_of(rows, first_row, total_rows) or rows
    first = first_row // size

    def kernel(*refs):
        refs[-1][...] = refs[0][...].T

    in_specs = [pl.BlockSpec((features, size), lambda i: (0, i))]
    operands = [wide]
    aliases = {}
    if base is not None:
        in_specs.append(pl.BlockSpec(memory_space=pl.ANY))
        operands.append(base)
        aliases = {1: 0}
    return pl.pallas_call(
        kernel,
        grid=(rows // size,),
        in_specs=in_specs,
        out_specs=pl.BlockSpec((size, features), lambda i: (first + i, 0)),
        out_shape=jax.ShapeDtypeStruct((total_rows, features), wide.dtype),
        input_output_aliases=aliases,
        cost_estimate=pl.CostEstimate(
            flops=0, bytes_accessed=4 * features * rows, transcendentals=0
        ),
    )(*operands)


def columns(wide, first, count, *others):
    size = block_of(first, count, *others)
    if size is None:
        return lax.slice_in_dim(wide, first, first + count, axis=1), count, 0
    return wide, size, first // size


def flip_product(wide, first, rows, chosen):
    features = wide.shape[0]
    wide, size, start = columns(wide, first, rows)
    slots = chosen.shape[0]

    def kernel(wide_ref, chosen_ref, rows_ref, product_ref):
        value = wide_ref[...]
        rows_ref[...] = value.T
        product_ref[...] = jnp.dot(chosen_ref[...], value, preferred_element_type=jnp.float32)

    return pl.pallas_call(
        kernel,
        grid=(rows // size,),
        in_specs=[
            pl.BlockSpec((features, size), lambda i: (0, start + i)),
            pl.BlockSpec((slots, features), lambda i: (0, 0)),
        ],
        out_specs=[
            pl.BlockSpec((size, features), lambda i: (i, 0)),
            pl.BlockSpec((slots, size), lambda i: (0, i)),
        ],
        out_shape=[
            jax.ShapeDtypeStruct((rows, features), wide.dtype),
            jax.ShapeDtypeStruct((slots, rows), jnp.float32),
        ],
        cost_estimate=pl.CostEstimate(
            flops=2 * slots * features * rows,
            bytes_accessed=4 * features * rows,
            transcendentals=0,
        ),
    )(wide, chosen)


def spread(train, gain):
    experts, features, count = train.shape
    rows = experts * count
    size = block_of(rows) or rows

    def kernel(train_ref, gain_ref, out_ref):
        out_ref[...] = (train_ref[...] * gain_ref[...]).astype(jnp.bfloat16).T

    return pl.pallas_call(
        kernel,
        grid=(rows // size,),
        in_specs=[
            pl.BlockSpec((size, features), lambda i: (i, 0)),
            pl.BlockSpec((1, features), lambda i: (0, 0)),
        ],
        out_specs=pl.BlockSpec((features, size), lambda i: (0, i)),
        out_shape=jax.ShapeDtypeStruct((features, rows), jnp.bfloat16),
        cost_estimate=pl.CostEstimate(
            flops=train.size, bytes_accessed=6 * train.size, transcendentals=0
        ),
    )(train.transpose(0, 2, 1).reshape(rows, features), gain[None, :])


def flip_dot(wide, first, total_rows, hidden):
    features = wide.shape[0]
    slots, rows = hidden.shape
    wide, size, start = columns(wide, first, rows, total_rows)

    def kernel(wide_ref, hidden_ref, rows_ref, total_ref):
        turned = wide_ref[...].T
        rows_ref[...] = turned

        @pl.when(pl.program_id(0) == 0)
        def _():
            total_ref[...] = jnp.zeros_like(total_ref)

        total_ref[...] += jnp.dot(hidden_ref[...], turned, preferred_element_type=jnp.float32)

    return pl.pallas_call(
        kernel,
        grid=(rows // size,),
        in_specs=[
            pl.BlockSpec((features, size), lambda i: (0, start + i)),
            pl.BlockSpec((slots, size), lambda i: (0, i)),
        ],
        out_specs=[
            pl.BlockSpec((size, features), lambda i: (i, 0)),
            pl.BlockSpec((slots, features), lambda i: (0, 0)),
        ],
        out_shape=[
            jax.ShapeDtypeStruct((total_rows, features), wide.dtype),
            jax.ShapeDtypeStruct((slots, features), jnp.float32),
        ],
        cost_estimate=pl.CostEstimate(
            flops=2 * slots * features * rows,
            bytes_accessed=4 * features * rows,
            transcendentals=0,
        ),
    )(wide, hidden)


def keep_dot(weights, chosen):
    rows, features = weights.shape
    size = block_of(rows) or rows
    slots = chosen.shape[0]

    def kernel(weights_ref, chosen_ref, rows_ref, product_ref):
        rows_ref[...] = weights_ref[...]
        product_ref[...] = lax.dot_general(
            chosen_ref[...],
            weights_ref[...],
            (((1,), (1,)), ((), ())),
            preferred_element_type=jnp.float32,
        )

    return pl.pallas_call(
        kernel,
        grid=(rows // size,),
        in_specs=[
            pl.BlockSpec((size, features), lambda i: (i, 0)),
            pl.BlockSpec((slots, features), lambda i: (0, 0)),
        ],
        out_specs=[
            pl.BlockSpec((size, features), lambda i: (i, 0)),
            pl.BlockSpec((slots, size), lambda i: (0, i)),
        ],
        out_shape=[
            jax.ShapeDtypeStruct((rows, features), weights.dtype),
            jax.ShapeDtypeStruct((slots, rows), jnp.float32),
        ],
        cost_estimate=pl.CostEstimate(
            flops=2 * slots * features * rows,
            bytes_accessed=4 * features * rows,
            transcendentals=0,
        ),
    )(weights, chosen)


def after(value, *others):
    def kernel(*refs):
        pass

    return pl.pallas_call(
        kernel,
        in_specs=[pl.BlockSpec(memory_space=pl.ANY)] * (1 + len(others)),
        out_specs=pl.BlockSpec(memory_space=pl.ANY),
        out_shape=jax.ShapeDtypeStruct(value.shape, value.dtype),
        input_output_aliases={0: 0},
    )(value, *others)


def shards(tokens, gate_train, up_train, down_train, gain, routes, route_weights):
    tp_count = lax.axis_size("tp")
    experts = gate_train.shape[0]
    slices = tp_count // experts
    gain_column = gain[None, :, None]
    up_round = (up_train * gain_column).astype(jnp.bfloat16)
    down_round = down_train.astype(jnp.bfloat16)

    def exchange(matrix):
        return lax.all_to_all(matrix, "tp", split_axis=0, concat_axis=1, tiled=True)

    gate_all = lax.all_gather(spread(gate_train, gain), "fs", axis=0, tiled=True)
    features = gate_all.shape[0]

    up_moved = exchange(arrange(up_round, tp_count))[0].T
    down_moved = exchange(arrange(down_round, tp_count))[0].T
    units = down_moved.shape[1]
    size = block_of(units) or units
    main = units - size if units > size else units
    both_wide = lax.all_gather(
        jnp.concatenate([up_moved, down_moved[:, :main]], axis=1), "fs", axis=0, tiled=True
    )

    tokens_wide = tokens.astype(jnp.float32)
    normed = (
        tokens_wide
        * lax.rsqrt(jnp.mean(tokens_wide * tokens_wide, axis=1, keepdims=True) + norm_eps)
    ).astype(jnp.bfloat16)
    expert = lax.axis_index("tp") // slices
    matches = routes == expert
    member = jnp.any(matches, axis=1)
    slot_index = jnp.cumsum(member.astype(jnp.int32)) - 1
    marked = jnp.where(member, slot_index, -1)
    picker = (marked[None, :] == jnp.arange(CAP, dtype=jnp.int32)[:, None]).astype(jnp.bfloat16)
    chosen = jnp.dot(picker, normed, preferred_element_type=jnp.float32).astype(jnp.bfloat16)
    contract_last = (((1,), (1,)), ((), ()))

    gate_moved = exchange(gate_all.reshape(features, tp_count, -1).transpose(1, 2, 0))
    gate_new, gate_pre = keep_dot(gate_moved[0], chosen)
    up_new, up_pre = flip_product(both_wide, 0, units, chosen)
    hidden = (jax.nn.silu(gate_pre) * up_pre).astype(jnp.bfloat16)
    down_new, partial_value = flip_dot(both_wide, units, units, hidden[:, :main])
    if main < units:
        rest_moved = after(down_moved[:, main:], gate_new)
        rest_wide = lax.all_gather(rest_moved, "fs", axis=0, tiled=True)
        partial_value = partial_value + lax.dot_general(
            hidden[:, main:], rest_wide, contract_last, preferred_element_type=jnp.float32
        )
        down_new = flip(rest_wide, units, main, down_new)
    partial_value = partial_value.astype(jnp.bfloat16)

    labels = jnp.arange(experts, dtype=jnp.int32)
    member_all = jnp.any(routes[:, :, None] == labels[None, None, :], axis=1)
    slots_all = jnp.cumsum(member_all.astype(jnp.int32), axis=0) - 1
    slot_pair = jnp.take_along_axis(slots_all, routes, axis=1)
    flat_index = slot_pair * experts + routes
    received = lax.all_to_all(
        partial_value.reshape(CAP, tp_count, -1), "tp", split_axis=1, concat_axis=1, tiled=True
    )
    summed = jnp.sum(received.reshape(CAP, experts, slices, -1).astype(jnp.float32), axis=2)
    summed = summed.reshape(CAP * experts, -1)
    picked = jnp.take(summed, flat_index, axis=0)
    mixed = jnp.sum(route_weights[:, :, None] * picked, axis=1)
    return (gate_new[None], up_new[None], down_new[None], mixed.astype(jnp.bfloat16))


def solution(mesh):
    in_specs = (
        P("fs", None),
        P(None, "fs", "tp"),
        P(None, "fs", "tp"),
        P(None, "fs", "tp"),
        P("fs"),
        P("fs", None),
        P("fs", None),
    )
    out_specs = (P("tp", None, None), P("tp", None, None), P("tp", None, None), P("fs", "tp"))
    return jax.shard_map(shards, mesh=mesh, in_specs=in_specs, out_specs=out_specs, check_vma=False)
```
